32 devices in a mesh: fs: 8 (over z, y), tp: 4 (over x, core).
Axes of the slice: x: 2, y: 2, z: 4, core: 2. Of those that a mesh axis runs over, the one named last changes fastest.
Arguments:
- prompt_tokens: bfloat16 [768, 4096], P('tp'), may hold values from -6 to 6
- norm_gain: float32 [4096], P('fs'), may hold values from 0.1 to 1.9
- gate_trained: float32 [4096, 11264], P('fs', 'tp'), may hold values from -0.09375 to 0.09375
- up_trained: float32 [4096, 11264], P('fs', 'tp'), may hold values from -0.09375 to 0.09375
- down_trained: float32 [11264, 4096], P('fs', 'tp'), may hold values from -0.078125 to 0.078125
Outputs:
- gate_serving: bfloat16 [4096, 11264], P(None, 'fs')
- up_serving: bfloat16 [4096, 11264], P(None, 'fs')
- down_serving: bfloat16 [11264, 4096], P('fs')
- mixed: bfloat16 [768, 4096], P('tp', 'fs')
The draws below stay inside these ranges and needn't reach their ends.
All inputs are finite; a program needn't handle non-finite values.
Results may differ from the reference program's by a relative error of at most 0.0082.
Values may be sent and summed in bfloat16 or wider, within the bound.
A program may use at most 128 MiB of HBM per device.

```python
import jax
import jax.numpy as jnp
from jax import lax

D = 4096
FF = 11264
TOKENS = 768


def with_spikes(entries, key, source, target, shards_of, factor):
    def block_of(dim):
        return (jnp.arange(entries.shape[dim]) // (entries.shape[dim] // shards_of)).reshape((-1,) + (1,) * (entries.ndim - 1 - dim))

    near = jax.random.permutation(key, shards_of)[block_of(target)]
    second = (block_of(target) + shards_of // 2) % shards_of
    return jnp.where((block_of(source) == near) | (block_of(source) == second), factor * entries, entries)


def levels(stream_key, extent, shards, low, high):
    def one(axis_at, blocks):
        heights = jax.random.uniform(jax.random.fold_in(jax.random.fold_in(stream_key, 6), axis_at), (blocks,), jnp.float32, low / len(shards), high / len(shards))
        return jnp.repeat(jnp.exp(heights), extent[axis_at] // blocks).reshape((-1,) + (1,) * (len(extent) - axis_at - 1))

    level = one(*shards[0])
    for cut in shards[1:]:
        level = level * one(*cut)
    return level


def scatter_about(stream_key, dims, scale, reach, cuts=(), dtype=jnp.bfloat16):
    entries = scale * jax.random.normal(stream_key, dims, jnp.float32)
    if cuts:
        entries = entries * levels(stream_key, dims, cuts, -0.22, 0.18)
    return jnp.clip(entries, -reach, reach).astype(dtype)


def heavy_noise(stream_key, dims, scale, bound, shards, heavy, dtype=jnp.bfloat16):
    values = scale * jax.random.normal(stream_key, dims, jnp.float32)
    if shards:
        values = values * levels(stream_key, dims, shards, -0.22, 0.18)
    return jnp.clip(with_spikes(values, jax.random.fold_in(stream_key, 3), *heavy), -bound, bound).astype(dtype)


def setup_inputs(seed: int = 0) -> dict:
    splits = jax.random.split(jax.random.key(seed), 6)
    return {
        "prompt_tokens": scatter_about(splits[0], (TOKENS, D), 1.0, 6.0, ((0, 4),)),
        "norm_gain": jnp.clip(1.0 + 0.18 * jax.random.normal(splits[1], (D,), jnp.float32), 0.1, 1.9),
        "gate_trained": scatter_about(splits[2], (D, FF), D ** -0.5, 0.09375, ((0, 8), (1, 4)), jnp.float32),
        "up_trained": scatter_about(splits[3], (D, FF), D ** -0.5, 0.09375, ((0, 8), (1, 4)), jnp.float32),
        "down_trained": heavy_noise(splits[4], (FF, D), FF ** -0.5, 0.078125, ((0, 8), (1, 4)), (0, 1, 8, 2.0), jnp.float32),
    }


def reference(prompt_tokens, norm_gain, gate_trained, up_trained, down_trained):
    gate_serving = (gate_trained * norm_gain[:, None]).astype(jnp.bfloat16)
    up_serving = (up_trained * norm_gain[:, None]).astype(jnp.bfloat16)
    down_serving = down_trained.astype(jnp.bfloat16)
    tokens = prompt_tokens.astype(jnp.float32)
    scale = jax.lax.rsqrt(lax.optimization_barrier(jnp.mean(tokens * tokens, axis=-1, keepdims=True)) + 1e-06)
    normed = (tokens * scale).astype(jnp.bfloat16)
    gate = jnp.dot(normed, gate_serving, preferred_element_type=jnp.float32)
    up = jnp.dot(normed, up_serving, preferred_element_type=jnp.float32)
    hidden = (jax.nn.silu(gate) * up).astype(jnp.bfloat16)
    mixed = jnp.dot(hidden, down_serving, preferred_element_type=jnp.float32).astype(jnp.bfloat16)
    return (gate_serving, up_serving, down_serving, mixed)
```

```python
import functools

import jax
import jax.numpy as jnp
from jax import lax
from jax.experimental import pallas as pl
from jax.experimental.pallas import tpu as pltpu
from jax.sharding import PartitionSpec as P

MESH = pl.DeviceIdType.MESH
HOME, AWAY, BOTH = 0, 1, 2


def chunk_plan(rows):
    unit = 16
    side = max(unit, rows * 5 // 32 // unit * unit)
    left = rows - 2 * side
    first = left // 2 // unit * unit
    sizes = ((side, AWAY), (side, HOME), (first, BOTH), (left - first, BOTH))
    plan, at = [], 0
    for size, way in sizes:
        plan.append((at, size, way))
        at += size
    return tuple(plan)


def exchange_kernel(fs, tp, plan, w, d, out, dout, part, wbuf, dbuf,
                    part_send, part_recv, own_send, relay_send, land_recv,
                    sib_send, sib_recv, cross_send, down_send, down_recv, local_sem):
    f, t = lax.axis_index("fs"), lax.axis_index("tp")
    x, c = t // 2, lax.rem(t, 2)
    rows, width = w.shape[1], out.shape[2]
    dcols = d.shape[1]
    sib, far = 2 * x + 1 - c, 2 * (1 - x) + c
    chunks = len(plan)

    me = f * tp + t
    barrier = pltpu.get_barrier_semaphore()
    for i in range(1, fs * tp):
        other = lax.rem(me + i, fs * tp)
        pl.semaphore_signal(barrier, inc=1, device_id=(other // tp, lax.rem(other, tp)), device_id_type=MESH)
    pl.semaphore_wait(barrier, fs * tp - 1)

    half = fs // 2
    own_cross = (f // half) != x
    part_cross = (f // half) == x
    true = f >= 0

    def uses(cross, way, dropped):
        return jnp.logical_not(cross) if way == dropped else true

    def remote(src, dst, ssem, rsem, fs_to, tp_to):
        return pltpu.make_async_remote_copy(
            src_ref=src, dst_ref=dst, send_sem=ssem, recv_sem=rsem,
            device_id=(fs_to, tp_to), device_id_type=MESH)

    sent = []

    def send(cond, copy):
        @pl.when(cond)
        def _():
            copy.start()
        sent.append((cond, copy))

    def to_serve(src, sems, k, cond, home):
        at, size, _ = plan[k]
        for y in range(2):
            to = 2 * home + y
            for g in range(2):
                here = jnp.logical_and(to == f, c == g)
                send(jnp.logical_and(cond, jnp.logical_not(here)), remote(
                    src.at[g, pl.ds(at, size), pl.ds(y * width, width)],
                    out.at[g, pl.ds(f * rows + at, size), :],
                    sems.at[g, y, k], land_recv.at[f, k], to, 2 * x + g))

    def part_copy(g, k):
        at, size, _ = plan[k]
        return remote(w.at[g, pl.ds(at, size), :], part.at[g, pl.ds(at, size), :],
                      part_send.at[g, k], part_recv.at[g, k], f, far)

    for k in range(chunks):
        for g in range(2):
            send(uses(own_cross, plan[k][2], HOME), part_copy(g, k))
    for k in range(chunks):
        to_serve(w, own_send, k, uses(own_cross, plan[k][2], AWAY), t)
    block = pl.ds(pl.multiple_of(t * dcols, dcols), dcols)
    down_far = remote(d, dout.at[:, block], down_send.at[0], down_recv.at[0], f, far)
    down_sib = remote(d, dout.at[:, block], down_send.at[1], down_recv.at[1], f, sib)
    send(true, down_far)
    send(true, down_sib)
    take = pltpu.make_async_copy(d, dbuf, local_sem.at[0])
    take.start()
    take.wait()
    put_down = pltpu.make_async_copy(dbuf, dout.at[:, block], local_sem.at[0])
    put_down.start()

    for k in range(chunks):
        come = uses(part_cross, plan[k][2], HOME)

        @pl.when(come)
        def _():
            for g in range(2):
                part_copy(g, k).wait_recv()
        to_serve(part, relay_send, k, come, lax.rem(t + 2, tp))

    keeps = lax.rem(f // 2, 2) == c
    at_home = (f // half) == x
    cols = pl.ds(pl.multiple_of(lax.rem(f, 2) * width, width), width)
    mine = pl.ds(f * rows, rows)
    put = pltpu.make_async_copy(wbuf, out.at[c, mine, :], local_sem.at[1])

    @pl.when(keeps)
    def _():
        @pl.when(at_home)
        def _():
            get = pltpu.make_async_copy(w.at[c, :, cols], wbuf, local_sem.at[1])
            get.start()
            get.wait()

        @pl.when(jnp.logical_not(at_home))
        def _():
            get = pltpu.make_async_copy(part.at[c, :, cols], wbuf, local_sem.at[1])
            get.start()
            get.wait()
        put.start()
        put.wait()

    def landed(g, k, source):
        at, size, _ = plan[k]
        return out.at[g, pl.ds(source * rows + at, size), :]

    def down_on():
        remote(d, dout.at[:, block], down_send.at[0], down_recv.at[0], f, far).wait_recv()
        fblock = pl.ds(pl.multiple_of(far * dcols, dcols), dcols)
        send(true, remote(dout.at[:, fblock], dout.at[:, fblock], down_send.at[2], down_recv.at[2], f, sib))

    for k in range(chunks):
        way = plan[k][2]
        if k == chunks - 1:
            down_on()
        for i in range(fs):
            source = i
            ref = landed(c, k, source)
            kept = jnp.logical_and(keeps, f == source)
            fwd = remote(ref, ref, sib_send.at[source, k], sib_recv.at[source, k], f, sib)
            crossed = remote(ref, ref, cross_send.at[source, k], land_recv.at[source, k], f, far)

            @pl.when(jnp.logical_not(kept))
            def _():
                crossed.wait_recv()
            send(true, fwd)
            if way != BOTH:
                turn = (source // half) != (f // half)
                side = at_home if way == HOME else jnp.logical_not(at_home)
                send(jnp.logical_and(turn, side), crossed)

    for k in range(chunks):
        for source in range(fs):
            ref = landed(1 - c, k, source)
            remote(ref, ref, sib_send.at[source, k], sib_recv.at[source, k], f, sib).wait_recv()
    put_down.wait()
    down_sib.wait_recv()
    remote(dout.at[:, block], dout.at[:, block], down_send.at[2], down_recv.at[2], f, sib).wait_recv()
    for cond, copy in sent:
        @pl.when(cond)
        def _():
            copy.wait_send()


def exchange(w, d, fs, tp):
    rows, wide = w.shape[1:]
    width = wide * tp // fs
    plan = chunk_plan(rows)
    n = len(plan)
    dma = pltpu.SemaphoreType.DMA
    any_space = pl.BlockSpec(memory_space=pl.ANY)
    return pl.pallas_call(
        functools.partial(exchange_kernel, fs, tp, plan),
        out_shape=(
            jax.ShapeDtypeStruct((2, rows * fs, width), w.dtype),
            jax.ShapeDtypeStruct((d.shape[0], d.shape[1] * tp), d.dtype),
            jax.ShapeDtypeStruct(w.shape, w.dtype),
        ),
        in_specs=[any_space] * 2,
        out_specs=(any_space,) * 3,
        scratch_shapes=[
            pltpu.VMEM((rows, width), w.dtype),
            pltpu.VMEM(d.shape, d.dtype),
            dma((2, n)), dma((2, n)), dma((2, 2, n)), dma((2, 2, n)), dma((fs, n)),
            dma((fs, n)), dma((fs, n)), dma((fs, n)), dma((3,)), dma((3,)), dma((2,)),
        ],
        compiler_params=pltpu.CompilerParams(collective_id=0, has_side_effects=True),
    )(w, d)


def gather_by_kernel(gate_cast, up_cast, down_cast):
    both, down_serving, _ = exchange(
        jnp.stack([gate_cast, up_cast]), down_cast, lax.axis_size("fs"), lax.axis_size("tp"))
    return both[0], both[1], down_serving


def gather_by_collectives(gate_cast, up_cast, down_cast):
    fs_count = lax.axis_size("fs")
    down_serving = lax.all_gather(down_cast, "tp", axis=1, tiled=True)

    def serve(cast):
        part = lax.all_to_all(cast, "tp", split_axis=0, concat_axis=1, tiled=True)
        mid = lax.all_to_all(part, "fs", split_axis=1, concat_axis=0, tiled=True)
        share, width = mid.shape[0] // fs_count, mid.shape[1]
        blocks = lax.all_gather(mid.reshape(fs_count, share, width), "tp", axis=1, tiled=True)
        return blocks.reshape(-1, width)

    return serve(gate_cast), serve(up_cast), down_serving


def on_device(prompt_tokens, norm_gain, gate_trained, up_trained, down_trained):
    fs, tp = lax.axis_size("fs"), lax.axis_size("tp")
    gate_cast = (gate_trained * norm_gain[:, None]).astype(jnp.bfloat16)
    up_cast = (up_trained * norm_gain[:, None]).astype(jnp.bfloat16)
    down_cast = down_trained.astype(jnp.bfloat16)
    routed = fs == 2 * tp and tp == 4
    gather = gather_by_kernel if routed else gather_by_collectives
    gate_serving, up_serving, down_serving = gather(gate_cast, up_cast, down_cast)
    tokens = prompt_tokens.astype(jnp.float32)
    scale = lax.rsqrt(jnp.mean(tokens * tokens, axis=-1, keepdims=True) + 1e-06)
    normed = (tokens * scale).astype(jnp.bfloat16)
    contract = (((0,), (1,)), ((), ()))
    gate_cols = lax.dot_general(gate_serving, normed, contract, preferred_element_type=jnp.float32)
    up_cols = lax.dot_general(up_serving, normed, contract, preferred_element_type=jnp.float32)
    hidden_cols = (jax.nn.silu(gate_cols) * up_cols).astype(jnp.bfloat16)
    summed = lax.psum_scatter(
        lax.dot_general(
            down_serving, hidden_cols, (((0,), (0,)), ((), ())), preferred_element_type=jnp.float32
        ),
        "fs",
        scatter_dimension=0,
        tiled=True,
    )
    mixed = summed.T.astype(jnp.bfloat16)
    return (gate_serving, up_serving, down_serving, mixed)


def solution(mesh):
    return jax.shard_map(
        on_device,
        mesh=mesh,
        in_specs=(P("tp", None), P("fs"), P("fs", "tp"), P("fs", "tp"), P("fs", "tp")),
        out_specs=(P(None, "fs"), P(None, "fs"), P("fs", None), P("tp", "fs")),
        check_vma=False,
    )
```

```python
import functools

import jax
import jax.numpy as jnp
from jax import lax
from jax.experimental import pallas as pl
from jax.experimental.pallas import tpu as pltpu
from jax.sharding import PartitionSpec as P

MESH = pl.DeviceIdType.MESH
HOME, AWAY, BOTH = 0, 1, 2


def chunk_plan(rows):
    unit = 16
    side = max(unit, rows * 5 // 32 // unit * unit)
    left = rows - 2 * side
    first = left // 2 // unit * unit
    sizes = ((side, AWAY), (side, HOME), (first, BOTH), (left - first, BOTH))
    plan, at = [], 0
    for size, way in sizes:
        plan.append((at, size, way))
        at += size
    return tuple(plan)


def exchange_kernel(fs, tp, plan, wg, wu, d, out, dout, part, wbuf, dbuf,
                    part_send, part_recv, own_send, relay_send, land_recv,
                    sib_send, sib_recv, cross_send, down_send, down_recv, local_sem):
    f, t = lax.axis_index("fs"), lax.axis_index("tp")
    x, c = t // 2, lax.rem(t, 2)
    w = (wg, wu)
    rows, width = wg.shape[0], out.shape[2]
    dcols = d.shape[1]
    sib, far = 2 * x + 1 - c, 2 * (1 - x) + c
    chunks = len(plan)

    me = f * tp + t
    barrier = pltpu.get_barrier_semaphore()
    for i in range(1, fs * tp):
        other = lax.rem(me + i, fs * tp)
        pl.semaphore_signal(barrier, inc=1, device_id=(other // tp, lax.rem(other, tp)), device_id_type=MESH)
    pl.semaphore_wait(barrier, fs * tp - 1)

    half = fs // 2
    own_cross = (f // half) != x
    part_cross = (f // half) == x
    true = f >= 0

    def uses(cross, way, dropped):
        return jnp.logical_not(cross) if way == dropped else true

    def remote(src, dst, ssem, rsem, fs_to, tp_to):
        return pltpu.make_async_remote_copy(
            src_ref=src, dst_ref=dst, send_sem=ssem, recv_sem=rsem,
            device_id=(fs_to, tp_to), device_id_type=MESH)

    sent = []

    def send(cond, copy):
        @pl.when(cond)
        def _():
            copy.start()
        sent.append((cond, copy))

    def to_serve(view, sems, k, cond, home):
        at, size, _ = plan[k]
        for y in range(2):
            to = 2 * home + y
            for g in range(2):
                here = jnp.logical_and(to == f, c == g)
                send(jnp.logical_and(cond, jnp.logical_not(here)), remote(
                    view(g, pl.ds(at, size), pl.ds(y * width, width)),
                    out.at[g, pl.ds(f * rows + at, size), :],
                    sems.at[g, y, k], land_recv.at[f, k], to, 2 * x + g))

    def part_copy(g, k):
        at, size, _ = plan[k]
        return remote(w[g].at[pl.ds(at, size), :], part.at[g, pl.ds(at, size), :],
                      part_send.at[g, k], part_recv.at[g, k], f, far)

    for k in range(chunks):
        for g in range(2):
            send(uses(own_cross, plan[k][2], HOME), part_copy(g, k))
    for k in range(chunks):
        to_serve(lambda g, r, q: w[g].at[r, q], own_send, k, uses(own_cross, plan[k][2], AWAY), t)
    block = pl.ds(pl.multiple_of(t * dcols, dcols), dcols)
    down_far = remote(d, dout.at[:, block], down_send.at[0], down_recv.at[0], f, far)
    down_sib = remote(d, dout.at[:, block], down_send.at[1], down_recv.at[1], f, sib)
    send(true, down_far)
    send(true, down_sib)
    take = pltpu.make_async_copy(d, dbuf, local_sem.at[0])
    take.start()
    take.wait()
    put_down = pltpu.make_async_copy(dbuf, dout.at[:, block], local_sem.at[0])
    put_down.start()

    for k in range(chunks):
        come = uses(part_cross, plan[k][2], HOME)

        @pl.when(come)
        def _():
            for g in range(2):
                part_copy(g, k).wait_recv()
        to_serve(lambda g, r, q: part.at[g, r, q], relay_send, k, come, lax.rem(t + 2, tp))

    keeps = lax.rem(f // 2, 2) == c
    at_home = (f // half) == x
    cols = pl.ds(pl.multiple_of(lax.rem(f, 2) * width, width), width)
    mine = pl.ds(f * rows, rows)
    put = pltpu.make_async_copy(wbuf, out.at[c, mine, :], local_sem.at[1])

    @pl.when(keeps)
    def _():
        for g in range(2):
            @pl.when(jnp.logical_and(at_home, c == g))
            def _():
                get = pltpu.make_async_copy(w[g].at[:, cols], wbuf, local_sem.at[1])
                get.start()
                get.wait()

        @pl.when(jnp.logical_not(at_home))
        def _():
            get = pltpu.make_async_copy(part.at[c, :, cols], wbuf, local_sem.at[1])
            get.start()
            get.wait()
        put.start()
        put.wait()

    def landed(g, k, source):
        at, size, _ = plan[k]
        return out.at[g, pl.ds(source * rows + at, size), :]

    def down_on():
        remote(d, dout.at[:, block], down_send.at[0], down_recv.at[0], f, far).wait_recv()
        fblock = pl.ds(pl.multiple_of(far * dcols, dcols), dcols)
        send(true, remote(dout.at[:, fblock], dout.at[:, fblock], down_send.at[2], down_recv.at[2], f, sib))

    def arrive(k, source, cond, cross):
        ref = landed(c, k, source)
        crossed = remote(ref, ref, cross_send.at[source, k], land_recv.at[source, k], f, far)
        kept = jnp.logical_and(keeps, f == source)

        @pl.when(jnp.logical_and(cond, jnp.logical_not(kept)))
        def _():
            crossed.wait_recv()
        if cross:
            send(cond, crossed)
        send(cond, remote(ref, ref, sib_send.at[source, k], sib_recv.at[source, k], f, sib))

    def turns(source):
        return (source // half) != (f // half)

    def side(k):
        return at_home if plan[k][2] == HOME else jnp.logical_not(at_home)

    one_way = [k for k in range(chunks) if plan[k][2] != BOTH]
    both_ways = [k for k in range(chunks) if plan[k][2] == BOTH]
    for k in one_way:
        for source in range(fs):
            arrive(k, source, jnp.logical_and(turns(source), side(k)), True)
    for k in one_way:
        for source in range(fs):
            arrive(k, source, jnp.logical_not(turns(source)), False)
    for k in both_ways:
        if k == both_ways[-1]:
            down_on()
        for source in range(fs):
            arrive(k, source, true, False)
    for k in one_way:
        for source in range(fs):
            arrive(k, source, jnp.logical_and(turns(source), jnp.logical_not(side(k))), False)

    for k in range(chunks):
        for source in range(fs):
            ref = landed(1 - c, k, source)
            remote(ref, ref, sib_send.at[source, k], sib_recv.at[source, k], f, sib).wait_recv()
    put_down.wait()
    down_sib.wait_recv()
    remote(dout.at[:, block], dout.at[:, block], down_send.at[2], down_recv.at[2], f, sib).wait_recv()
    for cond, copy in sent:
        @pl.when(cond)
        def _():
            copy.wait_send()


def exchange(wg, wu, d, fs, tp):
    rows, wide = wg.shape
    width = wide * tp // fs
    plan = chunk_plan(rows)
    n = len(plan)
    dma = pltpu.SemaphoreType.DMA
    any_space = pl.BlockSpec(memory_space=pl.ANY)
    return pl.pallas_call(
        functools.partial(exchange_kernel, fs, tp, plan),
        out_shape=(
            jax.ShapeDtypeStruct((2, rows * fs, width), wg.dtype),
            jax.ShapeDtypeStruct((d.shape[0], d.shape[1] * tp), d.dtype),
            jax.ShapeDtypeStruct((2, rows, wide), wg.dtype),
        ),
        in_specs=[any_space] * 3,
        out_specs=(any_space,) * 3,
        scratch_shapes=[
            pltpu.VMEM((rows, width), wg.dtype),
            pltpu.VMEM(d.shape, d.dtype),
            dma((2, n)), dma((2, n)), dma((2, 2, n)), dma((2, 2, n)), dma((fs, n)),
            dma((fs, n)), dma((fs, n)), dma((fs, n)), dma((3,)), dma((3,)), dma((2,)),
        ],
        compiler_params=pltpu.CompilerParams(collective_id=0, has_side_effects=True),
    )(wg, wu, d)


def hidden_kernel(tok, both, gate_out, up_out, hidden, acc, scale):
    i = pl.program_id(0)
    depth = gate_out.shape[0]

    @pl.when(i == 0)
    def _():
        t = tok[...].astype(jnp.float32)
        scale[...] = lax.rsqrt(jnp.mean(t * t, axis=-1, keepdims=True) + 1e-06)
        acc[...] = jnp.zeros_like(acc)

    gate_out[...] = both[0]
    up_out[...] = both[1]
    piece = tok[:, pl.ds(pl.multiple_of(i * depth, depth), depth)].astype(jnp.float32)
    normed = (piece * scale[...]).astype(jnp.bfloat16)
    for g in range(2):
        acc[g] += jnp.dot(normed, both[g], preferred_element_type=jnp.float32)

    @pl.when(i == pl.num_programs(0) - 1)
    def _():
        hidden[...] = (jax.nn.silu(acc[0]) * acc[1]).astype(hidden.dtype)


def hidden_units(tok, both, steps):
    _, features, width = both.shape
    depth = features // steps
    serving = jax.ShapeDtypeStruct((features, width), both.dtype)
    return pl.pallas_call(
        hidden_kernel,
        grid=(steps,),
        out_shape=(serving, serving, jax.ShapeDtypeStruct((tok.shape[0], width), both.dtype)),
        in_specs=[
            pl.BlockSpec(tok.shape, lambda i: (0, 0)),
            pl.BlockSpec((2, depth, width), lambda i: (0, i, 0)),
        ],
        out_specs=(
            pl.BlockSpec((depth, width), lambda i: (i, 0)),
            pl.BlockSpec((depth, width), lambda i: (i, 0)),
            pl.BlockSpec((tok.shape[0], width), lambda i: (0, 0)),
        ),
        scratch_shapes=[
            pltpu.VMEM((2, tok.shape[0], width), jnp.float32),
            pltpu.VMEM((tok.shape[0], 1), jnp.float32),
        ],
        compiler_params=pltpu.CompilerParams(dimension_semantics=("arbitrary",)),
    )(tok, both)


def partial_kernel(hidden, down, down_out, partial):
    down_out[...] = down[...]
    partial[0] = jnp.dot(hidden[...], down[...], preferred_element_type=jnp.float32).astype(partial.dtype)


def partial_sums(hidden, down, blocks):
    units, features = down.shape
    width = features // blocks
    return pl.pallas_call(
        partial_kernel,
        grid=(blocks,),
        out_shape=(
            jax.ShapeDtypeStruct(down.shape, down.dtype),
            jax.ShapeDtypeStruct((blocks, hidden.shape[0], width), jnp.bfloat16),
        ),
        in_specs=[
            pl.BlockSpec(hidden.shape, lambda j: (0, 0)),
            pl.BlockSpec((units, width), lambda j: (0, j)),
        ],
        out_specs=(
            pl.BlockSpec((units, width), lambda j: (0, j)),
            pl.BlockSpec((1, hidden.shape[0], width), lambda j: (j, 0, 0)),
        ),
        compiler_params=pltpu.CompilerParams(dimension_semantics=("arbitrary",)),
    )(hidden, down)


def reduce_kernel(fs, p, mixed, ybuf, sbuf, zbuf, ysend, yrecv, zsend, zrecv):
    f, t = lax.axis_index("fs"), lax.axis_index("tp")
    z, y = f // 2, lax.rem(f, 2)
    planes = fs // 2
    barrier = pltpu.get_barrier_semaphore()
    for i in range(1, fs):
        pl.semaphore_signal(barrier, inc=1, device_id=(lax.rem(f + i, fs), t), device_id_type=MESH)
    pl.semaphore_wait(barrier, fs - 1)

    def remote(src, dst, ssem, rsem, to):
        return pltpu.make_async_remote_copy(
            src_ref=src, dst_ref=dst, send_sem=ssem, recv_sem=rsem,
            device_id=(to, t), device_id_type=MESH)

    order = sorted(range(1, planes), key=lambda o: abs(o - planes // 2)) + [0]
    across, along = {}, {}
    for off in order:
        to = lax.rem(z + off, planes)
        across[off] = remote(p.at[2 * to + 1 - y], ybuf.at[off], ysend.at[off], yrecv.at[off], 2 * z + 1 - y)
        across[off].start()
    for off in order:
        to = lax.rem(z + off, planes)
        across[off].wait_recv()
        pair = p[2 * to + y].astype(jnp.float32) + ybuf[off].astype(jnp.float32)
        if off:
            sbuf[off] = pair.astype(sbuf.dtype)
            along[off] = remote(sbuf.at[off], zbuf.at[off], zsend.at[off], zrecv.at[off], 2 * to + y)
            along[off].start()
        else:
            total = pair
    for off in order[:-1]:
        along[off].wait_recv()
        total += zbuf[off].astype(jnp.float32)
    mixed[...] = total.astype(mixed.dtype)
    for off in order:
        across[off].wait_send()
        if off:
            along[off].wait_send()


def reduce_over_fs(p, fs):
    _, tokens, width = p.shape
    dma = pltpu.SemaphoreType.DMA
    slots = pltpu.VMEM((fs // 2, tokens, width), p.dtype)
    return pl.pallas_call(
        functools.partial(reduce_kernel, fs),
        out_shape=jax.ShapeDtypeStruct((tokens, width), jnp.bfloat16),
        in_specs=[pl.BlockSpec(memory_space=pltpu.VMEM)],
        out_specs=pl.BlockSpec(memory_space=pltpu.VMEM),
        scratch_shapes=[slots, slots, slots] + [dma((fs // 2,))] * 4,
        compiler_params=pltpu.CompilerParams(collective_id=1, has_side_effects=True),
    )(p)


def by_kernels(prompt_tokens, gate_cast, up_cast, down_cast):
    fs, tp = lax.axis_size("fs"), lax.axis_size("tp")
    both, down_all, _ = exchange(gate_cast, up_cast, down_cast, fs, tp)
    gate_serving, up_serving, hidden = hidden_units(prompt_tokens, both, fs)
    down_serving, partial = partial_sums(hidden, down_all, fs)
    return gate_serving, up_serving, down_serving, reduce_over_fs(partial, fs)


def gather_by_collectives(gate_cast, up_cast, down_cast):
    fs_count = lax.axis_size("fs")
    down_serving = lax.all_gather(down_cast, "tp", axis=1, tiled=True)

    def serve(cast):
        part = lax.all_to_all(cast, "tp", split_axis=0, concat_axis=1, tiled=True)
        mid = lax.all_to_all(part, "fs", split_axis=1, concat_axis=0, tiled=True)
        share, width = mid.shape[0] // fs_count, mid.shape[1]
        blocks = lax.all_gather(mid.reshape(fs_count, share, width), "tp", axis=1, tiled=True)
        return blocks.reshape(-1, width)

    return serve(gate_cast), serve(up_cast), down_serving


def on_device(prompt_tokens, norm_gain, gate_trained, up_trained, down_trained):
    fs, tp = lax.axis_size("fs"), lax.axis_size("tp")
    gate_cast = (gate_trained * norm_gain[:, None]).astype(jnp.bfloat16)
    up_cast = (up_trained * norm_gain[:, None]).astype(jnp.bfloat16)
    down_cast = down_trained.astype(jnp.bfloat16)
    routed = fs == 2 * tp and tp == 4
    if routed:
        return by_kernels(prompt_tokens, gate_cast, up_cast, down_cast)
    gate_serving, up_serving, down_serving = gather_by_collectives(gate_cast, up_cast, down_cast)
    tokens = prompt_tokens.astype(jnp.float32)
    scale = lax.rsqrt(jnp.mean(tokens * tokens, axis=-1, keepdims=True) + 1e-06)
    normed = (tokens * scale).astype(jnp.bfloat16)
    contract = (((0,), (1,)), ((), ()))
    gate_cols = lax.dot_general(gate_serving, normed, contract, preferred_element_type=jnp.float32)
    up_cols = lax.dot_general(up_serving, normed, contract, preferred_element_type=jnp.float32)
    hidden_cols = (jax.nn.silu(gate_cols) * up_cols).astype(jnp.bfloat16)
    summed = lax.psum_scatter(
        lax.dot_general(
            down_serving, hidden_cols, (((0,), (0,)), ((), ())), preferred_element_type=jnp.float32
        ),
        "fs",
        scatter_dimension=0,
        tiled=True,
    )
    mixed = summed.T.astype(jnp.bfloat16)
    return (gate_serving, up_serving, down_serving, mixed)


def solution(mesh):
    return jax.shard_map(
        on_device,
        mesh=mesh,
        in_specs=(P("tp", None), P("fs"), P("fs", "tp"), P("fs", "tp"), P("fs", "tp")),
        out_specs=(P(None, "fs"), P(None, "fs"), P("fs", None), P("tp", "fs")),
        check_vma=False,
    )
```

```python
import functools

import jax
import jax.numpy as jnp
from jax import lax
from jax.experimental import pallas as pl
from jax.experimental.pallas import tpu as pltpu
from jax.sharding import PartitionSpec as P

MESH = pl.DeviceIdType.MESH
HOME, AWAY, BOTH = 0, 1, 2


SHARES = ((1, AWAY), (2, BOTH), (4, AWAY), (7, HOME), (6, BOTH), (6, BOTH), (6, BOTH))


def chunk_plan(rows):
    unit = max(16, rows // sum(share for share, _ in SHARES) // 16 * 16)
    plan, at = [], 0
    for i, (share, way) in enumerate(SHARES):
        size = rows - at if i == len(SHARES) - 1 else share * unit
        plan.append((at, size, way))
        at += size
    return tuple(plan)


def exchange_kernel(fs, tp, plan, wg, wu, d, out, dout, part, wbuf, dbuf,
                    part_send, part_recv, own_send, relay_send, land_recv,
                    sib_send, sib_recv, cross_send, down_send, down_recv, local_sem):
    f, t = lax.axis_index("fs"), lax.axis_index("tp")
    x, c = t // 2, lax.rem(t, 2)
    w = (wg, wu)
    rows, width = wg.shape[0], out.shape[2]
    dcols = d.shape[1]
    sib, far = 2 * x + 1 - c, 2 * (1 - x) + c
    chunks = len(plan)

    me = f * tp + t
    barrier = pltpu.get_barrier_semaphore()
    for i in range(1, fs * tp):
        other = lax.rem(me + i, fs * tp)
        pl.semaphore_signal(barrier, inc=1, device_id=(other // tp, lax.rem(other, tp)), device_id_type=MESH)
    pl.semaphore_wait(barrier, fs * tp - 1)

    half = fs // 2
    own_cross = (f // half) != x
    part_cross = (f // half) == x
    true = f >= 0

    def uses(cross, way, dropped):
        return jnp.logical_not(cross) if way == dropped else true

    def remote(src, dst, ssem, rsem, fs_to, tp_to):
        return pltpu.make_async_remote_copy(
            src_ref=src, dst_ref=dst, send_sem=ssem, recv_sem=rsem,
            device_id=(fs_to, tp_to), device_id_type=MESH)

    sent = []

    def send(cond, copy):
        @pl.when(cond)
        def _():
            copy.start()
        sent.append((cond, copy))

    def to_serve(view, sems, k, cond, home):
        at, size, _ = plan[k]
        for y in range(2):
            to = 2 * home + y
            for g in range(2):
                here = jnp.logical_and(to == f, c == g)
                send(jnp.logical_and(cond, jnp.logical_not(here)), remote(
                    view(g, pl.ds(at, size), pl.ds(y * width, width)),
                    out.at[g, pl.ds(f * rows + at, size), :],
                    sems.at[g, y, k], land_recv.at[f, k], to, 2 * x + g))

    def part_copy(g, k):
        at, size, _ = plan[k]
        return remote(w[g].at[pl.ds(at, size), :], part.at[g, pl.ds(at, size), :],
                      part_send.at[g, k], part_recv.at[g, k], f, far)

    for k in range(chunks):
        for g in range(2):
            send(uses(own_cross, plan[k][2], HOME), part_copy(g, k))
    for k in range(chunks):
        to_serve(lambda g, r, q: w[g].at[r, q], own_send, k, uses(own_cross, plan[k][2], AWAY), t)
    block = pl.ds(pl.multiple_of(t * dcols, dcols), dcols)
    down_far = remote(d, dout.at[:, block], down_send.at[0], down_recv.at[0], f, far)
    down_sib = remote(d, dout.at[:, block], down_send.at[1], down_recv.at[1], f, sib)
    send(true, down_far)
    send(true, down_sib)
    take = pltpu.make_async_copy(d, dbuf, local_sem.at[0])
    take.start()
    take.wait()
    put_down = pltpu.make_async_copy(dbuf, dout.at[:, block], local_sem.at[0])
    put_down.start()

    for k in range(chunks):
        come = uses(part_cross, plan[k][2], HOME)

        @pl.when(come)
        def _():
            for g in range(2):
                part_copy(g, k).wait_recv()
        to_serve(lambda g, r, q: part.at[g, r, q], relay_send, k, come, lax.rem(t + 2, tp))

    keeps = lax.rem(f // 2, 2) == c
    at_home = (f // half) == x
    cols = pl.ds(pl.multiple_of(lax.rem(f, 2) * width, width), width)
    mine = pl.ds(f * rows, rows)
    put = pltpu.make_async_copy(wbuf, out.at[c, mine, :], local_sem.at[1])

    @pl.when(keeps)
    def _():
        for g in range(2):
            @pl.when(jnp.logical_and(at_home, c == g))
            def _():
                get = pltpu.make_async_copy(w[g].at[:, cols], wbuf, local_sem.at[1])
                get.start()
                get.wait()

        @pl.when(jnp.logical_not(at_home))
        def _():
            get = pltpu.make_async_copy(part.at[c, :, cols], wbuf, local_sem.at[1])
            get.start()
            get.wait()
        put.start()
        put.wait()

    def landed(g, k, source):
        at, size, _ = plan[k]
        return out.at[g, pl.ds(source * rows + at, size), :]

    def down_on():
        remote(d, dout.at[:, block], down_send.at[0], down_recv.at[0], f, far).wait_recv()
        fblock = pl.ds(pl.multiple_of(far * dcols, dcols), dcols)
        send(true, remote(dout.at[:, fblock], dout.at[:, fblock], down_send.at[2], down_recv.at[2], f, sib))

    def arrive(k, source, cond, cross):
        ref = landed(c, k, source)
        crossed = remote(ref, ref, cross_send.at[source, k], land_recv.at[source, k], f, far)
        kept = jnp.logical_and(keeps, f == source)

        @pl.when(jnp.logical_and(cond, jnp.logical_not(kept)))
        def _():
            crossed.wait_recv()
        if cross:
            send(cond, crossed)
        send(cond, remote(ref, ref, sib_send.at[source, k], sib_recv.at[source, k], f, sib))

    def turns(source):
        return (source // half) != (f // half)

    def side(k):
        return at_home if plan[k][2] == HOME else jnp.logical_not(at_home)

    one_way = [k for k in range(chunks) if plan[k][2] != BOTH]
    both_ways = [k for k in range(chunks) if plan[k][2] == BOTH]
    for k in one_way:
        for source in range(fs):
            arrive(k, source, jnp.logical_and(turns(source), side(k)), True)
    for k in one_way:
        for source in range(fs):
            arrive(k, source, jnp.logical_not(turns(source)), False)
    for k in both_ways:
        if k == both_ways[-1]:
            down_on()
        for source in range(fs):
            arrive(k, source, true, False)
    for k in one_way:
        for source in range(fs):
            arrive(k, source, jnp.logical_and(turns(source), jnp.logical_not(side(k))), False)

    for k in range(chunks):
        for source in range(fs):
            ref = landed(1 - c, k, source)
            remote(ref, ref, sib_send.at[source, k], sib_recv.at[source, k], f, sib).wait_recv()
    put_down.wait()
    down_sib.wait_recv()
    remote(dout.at[:, block], dout.at[:, block], down_send.at[2], down_recv.at[2], f, sib).wait_recv()
    for cond, copy in sent:
        @pl.when(cond)
        def _():
            copy.wait_send()


def exchange(wg, wu, d, fs, tp):
    rows, wide = wg.shape
    width = wide * tp // fs
    plan = chunk_plan(rows)
    n = len(plan)
    dma = pltpu.SemaphoreType.DMA
    any_space = pl.BlockSpec(memory_space=pl.ANY)
    return pl.pallas_call(
        functools.partial(exchange_kernel, fs, tp, plan),
        out_shape=(
            jax.ShapeDtypeStruct((2, rows * fs, width), wg.dtype),
            jax.ShapeDtypeStruct((d.shape[0], d.shape[1] * tp), d.dtype),
            jax.ShapeDtypeStruct((2, rows, wide), wg.dtype),
        ),
        in_specs=[any_space] * 3,
        out_specs=(any_space,) * 3,
        scratch_shapes=[
            pltpu.VMEM((rows, width), wg.dtype),
            pltpu.VMEM(d.shape, d.dtype),
            dma((2, n)), dma((2, n)), dma((2, 2, n)), dma((2, 2, n)), dma((fs, n)),
            dma((fs, n)), dma((fs, n)), dma((fs, n)), dma((3,)), dma((3,)), dma((2,)),
        ],
        compiler_params=pltpu.CompilerParams(collective_id=0, has_side_effects=True),
    )(wg, wu, d)


def hidden_kernel(tok, both, gate_out, up_out, hidden, acc, scale):
    i = pl.program_id(0)
    depth = gate_out.shape[0]

    @pl.when(i == 0)
    def _():
        t = tok[...].astype(jnp.float32)
        scale[...] = lax.rsqrt(jnp.mean(t * t, axis=-1, keepdims=True) + 1e-06)
        acc[...] = jnp.zeros_like(acc)

    gate_out[...] = both[0]
    up_out[...] = both[1]
    piece = tok[:, pl.ds(pl.multiple_of(i * depth, depth), depth)].astype(jnp.float32)
    normed = (piece * scale[...]).astype(jnp.bfloat16)
    for g in range(2):
        acc[g] += jnp.dot(normed, both[g], preferred_element_type=jnp.float32)

    @pl.when(i == pl.num_programs(0) - 1)
    def _():
        hidden[...] = (jax.nn.silu(acc[0]) * acc[1]).astype(hidden.dtype)


def hidden_units(tok, both, steps):
    _, features, width = both.shape
    depth = features // steps
    serving = jax.ShapeDtypeStruct((features, width), both.dtype)
    return pl.pallas_call(
        hidden_kernel,
        grid=(steps,),
        out_shape=(serving, serving, jax.ShapeDtypeStruct((tok.shape[0], width), both.dtype)),
        in_specs=[
            pl.BlockSpec(tok.shape, lambda i: (0, 0)),
            pl.BlockSpec((2, depth, width), lambda i: (0, i, 0)),
        ],
        out_specs=(
            pl.BlockSpec((depth, width), lambda i: (i, 0)),
            pl.BlockSpec((depth, width), lambda i: (i, 0)),
            pl.BlockSpec((tok.shape[0], width), lambda i: (0, 0)),
        ),
        scratch_shapes=[
            pltpu.VMEM((2, tok.shape[0], width), jnp.float32),
            pltpu.VMEM((tok.shape[0], 1), jnp.float32),
        ],
        compiler_params=pltpu.CompilerParams(dimension_semantics=("arbitrary",)),
    )(tok, both)


def partial_kernel(hidden, down, down_out, partial):
    down_out[...] = down[...]
    partial[0] = jnp.dot(hidden[...], down[...], preferred_element_type=jnp.float32).astype(partial.dtype)


def partial_sums(hidden, down, blocks):
    units, features = down.shape
    width = features // blocks
    return pl.pallas_call(
        partial_kernel,
        grid=(blocks,),
        out_shape=(
            jax.ShapeDtypeStruct(down.shape, down.dtype),
            jax.ShapeDtypeStruct((blocks, hidden.shape[0], width), jnp.bfloat16),
        ),
        in_specs=[
            pl.BlockSpec(hidden.shape, lambda j: (0, 0)),
            pl.BlockSpec((units, width), lambda j: (0, j)),
        ],
        out_specs=(
            pl.BlockSpec((units, width), lambda j: (0, j)),
            pl.BlockSpec((1, hidden.shape[0], width), lambda j: (j, 0, 0)),
        ),
        compiler_params=pltpu.CompilerParams(dimension_semantics=("arbitrary",)),
    )(hidden, down)


def reduce_kernel(fs, p, mixed, ybuf, sbuf, zbuf, ysend, yrecv, zsend, zrecv):
    f, t = lax.axis_index("fs"), lax.axis_index("tp")
    z, y = f // 2, lax.rem(f, 2)
    planes = fs // 2
    barrier = pltpu.get_barrier_semaphore()
    for i in range(1, fs):
        pl.semaphore_signal(barrier, inc=1, device_id=(lax.rem(f + i, fs), t), device_id_type=MESH)
    pl.semaphore_wait(barrier, fs - 1)

    def remote(src, dst, ssem, rsem, to):
        return pltpu.make_async_remote_copy(
            src_ref=src, dst_ref=dst, send_sem=ssem, recv_sem=rsem,
            device_id=(to, t), device_id_type=MESH)

    order = sorted(range(1, planes), key=lambda o: abs(o - planes // 2)) + [0]
    across, along = {}, {}
    for off in order:
        to = lax.rem(z + off, planes)
        across[off] = remote(p.at[2 * to + 1 - y], ybuf.at[off], ysend.at[off], yrecv.at[off], 2 * z + 1 - y)
        across[off].start()
    for off in order:
        to = lax.rem(z + off, planes)
        across[off].wait_recv()
        pair = p[2 * to + y].astype(jnp.float32) + ybuf[off].astype(jnp.float32)
        if off:
            sbuf[off] = pair.astype(sbuf.dtype)
            along[off] = remote(sbuf.at[off], zbuf.at[off], zsend.at[off], zrecv.at[off], 2 * to + y)
            along[off].start()
        else:
            total = pair
    for off in order[:-1]:
        along[off].wait_recv()
        total += zbuf[off].astype(jnp.float32)
    mixed[...] = total.astype(mixed.dtype)
    for off in order:
        across[off].wait_send()
        if off:
            along[off].wait_send()


def reduce_over_fs(p, fs):
    _, tokens, width = p.shape
    dma = pltpu.SemaphoreType.DMA
    slots = pltpu.VMEM((fs // 2, tokens, width), p.dtype)
    return pl.pallas_call(
        functools.partial(reduce_kernel, fs),
        out_shape=jax.ShapeDtypeStruct((tokens, width), jnp.bfloat16),
        in_specs=[pl.BlockSpec(memory_space=pltpu.VMEM)],
        out_specs=pl.BlockSpec(memory_space=pltpu.VMEM),
        scratch_shapes=[slots, slots, slots] + [dma((fs // 2,))] * 4,
        compiler_params=pltpu.CompilerParams(collective_id=1, has_side_effects=True),
    )(p)


def by_kernels(prompt_tokens, gate_cast, up_cast, down_cast):
    fs, tp = lax.axis_size("fs"), lax.axis_size("tp")
    both, down_all, _ = exchange(gate_cast, up_cast, down_cast, fs, tp)
    gate_serving, up_serving, hidden = hidden_units(prompt_tokens, both, fs)
    down_serving, partial = partial_sums(hidden, down_all, fs)
    return gate_serving, up_serving, down_serving, reduce_over_fs(partial, fs)


def gather_by_collectives(gate_cast, up_cast, down_cast):
    fs_count = lax.axis_size("fs")
    down_serving = lax.all_gather(down_cast, "tp", axis=1, tiled=True)

    def serve(cast):
        part = lax.all_to_all(cast, "tp", split_axis=0, concat_axis=1, tiled=True)
        mid = lax.all_to_all(part, "fs", split_axis=1, concat_axis=0, tiled=True)
        share, width = mid.shape[0] // fs_count, mid.shape[1]
        blocks = lax.all_gather(mid.reshape(fs_count, share, width), "tp", axis=1, tiled=True)
        return blocks.reshape(-1, width)

    return serve(gate_cast), serve(up_cast), down_serving


def on_device(prompt_tokens, norm_gain, gate_trained, up_trained, down_trained):
    fs, tp = lax.axis_size("fs"), lax.axis_size("tp")
    gate_cast = (gate_trained * norm_gain[:, None]).astype(jnp.bfloat16)
    up_cast = (up_trained * norm_gain[:, None]).astype(jnp.bfloat16)
    down_cast = down_trained.astype(jnp.bfloat16)
    routed = fs == 2 * tp and tp == 4
    if routed:
        return by_kernels(prompt_tokens, gate_cast, up_cast, down_cast)
    gate_serving, up_serving, down_serving = gather_by_collectives(gate_cast, up_cast, down_cast)
    tokens = prompt_tokens.astype(jnp.float32)
    scale = lax.rsqrt(jnp.mean(tokens * tokens, axis=-1, keepdims=True) + 1e-06)
    normed = (tokens * scale).astype(jnp.bfloat16)
    contract = (((0,), (1,)), ((), ()))
    gate_cols = lax.dot_general(gate_serving, normed, contract, preferred_element_type=jnp.float32)
    up_cols = lax.dot_general(up_serving, normed, contract, preferred_element_type=jnp.float32)
    hidden_cols = (jax.nn.silu(gate_cols) * up_cols).astype(jnp.bfloat16)
    summed = lax.psum_scatter(
        lax.dot_general(
            down_serving, hidden_cols, (((0,), (0,)), ((), ())), preferred_element_type=jnp.float32
        ),
        "fs",
        scatter_dimension=0,
        tiled=True,
    )
    mixed = summed.T.astype(jnp.bfloat16)
    return (gate_serving, up_serving, down_serving, mixed)


def solution(mesh):
    return jax.shard_map(
        on_device,
        mesh=mesh,
        in_specs=(P("tp", None), P("fs"), P("fs", "tp"), P("fs", "tp"), P("fs", "tp")),
        out_specs=(P(None, "fs"), P(None, "fs"), P("fs", None), P("tp", "fs")),
        check_vma=False,
    )
```
